32 devices in a mesh: fs: 8 (over z, x), tp: 4 (over y, core).
Axes of the slice: x: 2, y: 2, z: 4, core: 2. Of those that a mesh axis runs over, the one named last changes fastest.
Arguments:
- resid: bfloat16 [8192, 2048], P(('fs', 'tp')), may hold values from -6 to 6
- mix_gain: float32 [2048], replicated, may hold values from 0.1 to 1.9
- in_weight: bfloat16 [2048, 2048], P('fs', 'tp'), may hold values from -0.125 to 0.125
- conv_taps: float32 [4, 2048], P(None, 'tp'), may hold values from -3 to 3
- recur_gate_w: bfloat16 [32, 64, 64], P('tp'), may hold values from -0.75 to 0.75
- input_gate_w: bfloat16 [32, 64, 64], P('tp'), may hold values from -0.75 to 0.75
- decay_rate: float32 [2048], P('tp'), may hold values from 0.0004 to 0.03
- out_weight: bfloat16 [2048, 2048], P('tp', 'fs'), may hold values from -0.25 to 0.25
- mlp_gain: float32 [2048], replicated, may hold values from 0.1 to 1.9
- up_gate_w: bfloat16 [2048, 5632], P('fs', 'tp'), may hold values from -0.125 to 0.125
- up_val_w: bfloat16 [2048, 5632], P('fs', 'tp'), may hold values from -0.125 to 0.125
- ffn_taps: float32 [3, 5632], P(None, 'tp'), may hold values from -3 to 3
- down_weight: bfloat16 [5632, 2048], P('tp', 'fs'), may hold values from -0.15625 to 0.15625
Outputs:
- result: bfloat16 [8192, 2048], P(('fs', 'tp'))
The draws below stay inside these ranges and needn't reach their ends.
All inputs are finite; a program needn't handle non-finite values.
Results may differ from the reference program's by a relative error of at most 0.028.
Values may be sent and summed in bfloat16 or wider, within the bound.
A program may use at most 64 MiB of HBM per device.

```python
import math
import jax
import jax.numpy as jnp
from jax import lax

D = 2048
RECUR = 2048
HIDDEN_SIZE = 5632
GATE_BLOCK = 64
SEQ_LEN = 128
NBLOCKS = 32
TOKENS = 8192
N_TP = 4


def block_levels(stream_key, dims, pieces, low, high):
    gain = 1.0
    for position, parts in pieces:
        heights = jax.random.uniform(jax.random.fold_in(jax.random.fold_in(stream_key, 6), position), (parts,), jnp.float32, low / len(pieces), high / len(pieces))
        gain = gain * jnp.repeat(jnp.exp(heights), dims[position] // parts).reshape((-1,) + (1,) * (len(dims) - 1 - position))
    return gain


def noise(rng, dims, spread, reach, shards=(), kind=jnp.bfloat16):
    level = block_levels(rng, dims, shards, -0.22, 0.18) if shards else 1.0
    drawn = jax.random.normal(rng, dims, jnp.float32) * spread * level
    return jnp.minimum(jnp.maximum(drawn, -reach), reach).astype(kind)


def setup_inputs(seed: int = 0) -> dict:
    splits = jax.random.split(jax.random.key(seed), 14)
    return {
        "resid": noise(splits[0], (TOKENS, D), 1.0, 6.0, ((0, 32),)),
        "mix_gain": jnp.clip(1.0 + 0.18 * jax.random.normal(splits[1], (D,), jnp.float32), 0.1, 1.9),
        "in_weight": noise(splits[2], (D, RECUR), D ** -0.5, 0.125, ((0, 8), (1, 4))),
        "conv_taps": noise(splits[3], (4, RECUR), 0.5, 3.0, ((1, 4),), jnp.float32),
        "recur_gate_w": noise(splits[4], (NBLOCKS, GATE_BLOCK, GATE_BLOCK), GATE_BLOCK ** -0.5, 0.75, ((0, 4),)),
        "input_gate_w": noise(splits[5], (NBLOCKS, GATE_BLOCK, GATE_BLOCK), GATE_BLOCK ** -0.5, 0.75, ((0, 4),)),
        "decay_rate": jnp.clip(jnp.exp(math.log(0.03) - 4.317488 * jax.random.uniform(splits[6], (RECUR,), jnp.float32) ** block_levels(splits[6], (RECUR,), ((0, 4),), -0.2, 0.2)), 0.0004, 0.03),
        "out_weight": noise(splits[7], (RECUR, D), (RECUR // 4) ** -0.5, 0.25, ((0, 4), (1, 8))),
        "mlp_gain": jnp.clip(1.0 + 0.18 * jax.random.normal(splits[8], (D,), jnp.float32), 0.1, 1.9),
        "up_gate_w": noise(splits[9], (D, HIDDEN_SIZE), D ** -0.5, 0.125, ((0, 8), (1, 4))),
        "up_val_w": noise(splits[10], (D, HIDDEN_SIZE), D ** -0.5, 0.125, ((0, 8), (1, 4))),
        "ffn_taps": noise(splits[11], (3, HIDDEN_SIZE), 0.6, 3.0, ((1, 4),), jnp.float32),
        "down_weight": noise(splits[12], (HIDDEN_SIZE, D), (HIDDEN_SIZE // 4) ** -0.5, 0.15625, ((0, 4), (1, 8))),
    }


def rms_scale(rows_in, gain_vec):
    wide = rows_in.astype(jnp.float32)
    return wide * lax.rsqrt(lax.optimization_barrier(jnp.mean(wide * wide, axis=-1, keepdims=True)) + 1e-06) * gain_vec

def causal_taps(values, tap_weights):
    width = tap_weights.shape[0]
    length = values.shape[1]
    padded = jnp.pad(values, ((0, 0), (width - 1, 0), (0, 0)))
    summed = jnp.zeros_like(values)
    for tap_index in range(width):
        summed = summed + padded[:, tap_index:tap_index + length] * tap_weights[tap_index]
    return summed

def combine(earlier, later):
    return (earlier[0] * later[0], later[0] * earlier[1] + later[1])

def group_sum(left, right, groups):
    step_size = left.shape[1] // groups
    summed = jnp.zeros((left.shape[0], right.shape[1]), jnp.float32)
    for group in range(groups):
        term = jnp.dot(left[:, group * step_size:(group + 1) * step_size], right[group * step_size:(group + 1) * step_size], preferred_element_type=jnp.float32)
        term = lax.optimization_barrier(term.astype(jnp.bfloat16))
        summed = summed + term.astype(jnp.float32)
    return summed

def reference(resid, mix_gain, in_weight, conv_taps, recur_gate_w, input_gate_w, decay_rate, out_weight, mlp_gain, up_gate_w, up_val_w, ffn_taps, down_weight):
    seqs = TOKENS // SEQ_LEN
    normed = rms_scale(resid, mix_gain).astype(jnp.bfloat16)
    projected = jnp.dot(normed, in_weight, preferred_element_type=jnp.float32).astype(jnp.bfloat16)
    conv = causal_taps(projected.astype(jnp.float32).reshape(seqs, SEQ_LEN, RECUR), conv_taps)
    blocks = conv.astype(jnp.bfloat16).astype(jnp.float32).reshape(seqs, SEQ_LEN, NBLOCKS, GATE_BLOCK)
    rgate = jax.nn.sigmoid(jnp.einsum('slnd,nde->slne', blocks, recur_gate_w.astype(jnp.float32)).reshape(seqs, SEQ_LEN, RECUR))
    igate = jax.nn.sigmoid(jnp.einsum('slnd,nde->slne', blocks, input_gate_w.astype(jnp.float32)).reshape(seqs, SEQ_LEN, RECUR))
    logdecay = -8.0 * rgate * decay_rate
    decay = jnp.exp(logdecay)
    drive = jnp.sqrt(-jnp.expm1(2.0 * logdecay)) * (igate * conv)
    state = lax.associative_scan(combine, (decay, drive), axis=1)[1]
    recurred = state.astype(jnp.bfloat16).reshape(TOKENS, RECUR)
    mixed_sum = group_sum(recurred, out_weight, N_TP)
    middle = (resid.astype(jnp.float32) + mixed_sum).astype(jnp.bfloat16)
    normed_two = rms_scale(middle, mlp_gain).astype(jnp.bfloat16)
    gate_pre = jnp.dot(normed_two, up_gate_w, preferred_element_type=jnp.float32).astype(jnp.bfloat16)
    value_pre = jnp.dot(normed_two, up_val_w, preferred_element_type=jnp.float32).astype(jnp.bfloat16)
    gate_conv = causal_taps(gate_pre.astype(jnp.float32).reshape(seqs, SEQ_LEN, HIDDEN_SIZE), ffn_taps).reshape(TOKENS, HIDDEN_SIZE)
    hidden = (jax.nn.silu(gate_conv) * value_pre.astype(jnp.float32)).astype(jnp.bfloat16)
    ffn_sum = group_sum(hidden, down_weight, N_TP)
    return (middle.astype(jnp.float32) + ffn_sum).astype(jnp.bfloat16)
```

```python
import functools

import jax
import jax.numpy as jnp
from jax import lax
from jax.experimental import pallas as pl
from jax.experimental.pallas import tpu as pltpu
from jax.sharding import PartitionSpec as P

GATE_BLOCK = 64
SEQ_LEN = 128
LANES = 128
CORES = 2


def rms_scale(rows_in, gain_vec):
    wide = rows_in.astype(jnp.float32)
    return wide * lax.rsqrt(jnp.mean(wide * wide, axis=-1, keepdims=True) + 1e-06) * gain_vec


def causal_taps(values, tap_weights):
    width = tap_weights.shape[0]
    length = values.shape[1]
    padded = jnp.pad(values, ((0, 0), (width - 1, 0), (0, 0)))
    summed = jnp.zeros_like(values)
    for tap_index in range(width):
        summed = summed + padded[:, tap_index : tap_index + length] * tap_weights[tap_index]
    return summed


def negative_expm1(arg):
    series = jnp.ones_like(arg)
    for order in range(8, 1, -1):
        series = 1.0 + arg * (1.0 / order) * series
    return jnp.where(arg > -0.5, -arg * series, 1.0 - jnp.exp(arg))


def shift_rows(values, distance, rows, fill):
    return jnp.where(rows >= distance, pltpu.roll(values, distance, 0), fill)


def recurrence_kernel(projected_ref, taps_ref, gates_ref, rate_ref, out_ref):
    width = taps_ref.shape[0]
    rows = lax.broadcasted_iota(jnp.int32, (SEQ_LEN, LANES), 0)
    for chunk in range(projected_ref.shape[1] // LANES):
        cols = slice(chunk * LANES, (chunk + 1) * LANES)
        values = projected_ref[:, cols].astype(jnp.float32)
        conv = values * taps_ref[width - 1 : width, cols]
        for back in range(1, width):
            tap = taps_ref[width - 1 - back : width - back, cols]
            conv = conv + shift_rows(values, back, rows, 0.0) * tap
        gates = jax.nn.sigmoid(
            jnp.dot(
                conv.astype(jnp.bfloat16), gates_ref[chunk], preferred_element_type=jnp.float32
            )
        )
        rgate = gates[:, :LANES]
        igate = gates[:, LANES:]
        logdecay = -8.0 * rgate * rate_ref[:, cols]
        decay = jnp.exp(logdecay)
        state = jnp.sqrt(negative_expm1(2.0 * logdecay)) * (igate * conv)
        distance = 1
        while distance < SEQ_LEN:
            state = state + decay * shift_rows(state, distance, rows, 0.0)
            if 2 * distance < SEQ_LEN:
                decay = decay * shift_rows(decay, distance, rows, 1.0)
            distance *= 2
        out_ref[:, cols] = state.astype(jnp.bfloat16)


def pair_blocks(blocks):
    pairs = blocks.reshape(-1, 2, GATE_BLOCK, GATE_BLOCK)
    blank = jnp.zeros_like(pairs[:, 0])
    upper = jnp.concatenate([pairs[:, 0], blank], axis=2)
    lower = jnp.concatenate([blank, pairs[:, 1]], axis=2)
    return jnp.concatenate([upper, lower], axis=1)


def recurrence(projected, conv_taps, gates, decay_rate):
    count, channels = projected.shape
    whole = lambda shape: pl.BlockSpec(shape, lambda seq: (0,) * len(shape))
    return pl.pallas_call(
        recurrence_kernel,
        grid=(count // SEQ_LEN,),
        in_specs=[
            pl.BlockSpec((SEQ_LEN, channels), lambda seq: (seq, 0)),
            whole(conv_taps.shape),
            whole(gates.shape),
            whole((1, channels)),
        ],
        out_specs=pl.BlockSpec((SEQ_LEN, channels), lambda seq: (seq, 0)),
        out_shape=jax.ShapeDtypeStruct(projected.shape, jnp.bfloat16),
        cost_estimate=pl.CostEstimate(
            flops=count * channels * 600, bytes_accessed=count * channels * 4,
            transcendentals=count * channels * 6,
        ),
    )(projected, conv_taps, gates, decay_rate.reshape(1, channels))


def gather_groups(block, n_tp):
    sides = n_tp // CORES
    swap = [(i, i ^ 1) for i in range(n_tp)]
    groups = []
    for distance in range(sides):
        mine = block
        if distance:
            back = [
                (i, ((i // CORES - distance) % sides) * CORES + i % CORES) for i in range(n_tp)
            ]
            mine = lax.ppermute(block, "tp", back)
        groups.append(jnp.concatenate([mine, lax.ppermute(mine, "tp", swap)], axis=0))
    return groups


def scatter_sum(partial_of, n_tp):
    sides = n_tp // CORES
    swap = [(i, i ^ 1) for i in range(n_tp)]
    total = 0.0
    for distance in reversed(range(sides)):
        partial = partial_of(distance)
        half = partial.shape[0] // 2
        other = lax.ppermute(partial[half:], "tp", swap)
        pair = partial[:half].astype(jnp.float32) + other.astype(jnp.float32)
        if distance:
            ahead = [
                (i, ((i // CORES + distance) % sides) * CORES + i % CORES) for i in range(n_tp)
            ]
            pair = lax.ppermute(pair.astype(jnp.bfloat16), "tp", ahead).astype(jnp.float32)
        total = total + pair
    return total


def dot(left, right):
    return jnp.dot(left, right, preferred_element_type=jnp.float32).astype(jnp.bfloat16)


def shards(
    n_tp,
    resid,
    mix_gain,
    in_weight,
    conv_taps,
    recur_gate_w,
    input_gate_w,
    decay_rate,
    out_weight,
    mlp_gain,
    up_gate_w,
    up_val_w,
    ffn_taps,
    down_weight,
):
    in_full = lax.all_gather(in_weight, "fs", axis=0, tiled=True)
    out_full = lax.all_gather(out_weight, "fs", axis=1, tiled=True)
    gate_full = lax.all_gather(up_gate_w, "fs", axis=0, tiled=True)
    val_full = lax.all_gather(up_val_w, "fs", axis=0, tiled=True)
    down_full = lax.all_gather(down_weight, "fs", axis=1, tiled=True)
    gates = jnp.concatenate([pair_blocks(recur_gate_w), pair_blocks(input_gate_w)], axis=2)

    normed = rms_scale(resid, mix_gain).astype(jnp.bfloat16)
    recurred = [
        recurrence(dot(rows, in_full), conv_taps, gates, decay_rate)
        for rows in gather_groups(normed, n_tp)
    ]
    mixed_sum = scatter_sum(lambda distance: dot(recurred[distance], out_full), n_tp)
    middle = (resid.astype(jnp.float32) + mixed_sum).astype(jnp.bfloat16)
    normed_two = rms_scale(middle, mlp_gain).astype(jnp.bfloat16)

    hidden = []
    for rows in gather_groups(normed_two, n_tp):
        gate_pre = dot(rows, gate_full)
        value_pre = dot(rows, val_full)
        seqs = gate_pre.shape[0] // SEQ_LEN
        gate_conv = causal_taps(
            gate_pre.astype(jnp.float32).reshape(seqs, SEQ_LEN, -1), ffn_taps
        ).reshape(gate_pre.shape)
        hidden.append((jax.nn.silu(gate_conv) * value_pre.astype(jnp.float32)).astype(jnp.bfloat16))
    ffn_sum = scatter_sum(lambda distance: dot(hidden[distance], down_full), n_tp)
    return (middle.astype(jnp.float32) + ffn_sum).astype(jnp.bfloat16)


def solution(mesh):
    in_specs = (
        P(("fs", "tp"), None),
        P(),
        P("fs", "tp"),
        P(None, "tp"),
        P("tp", None, None),
        P("tp", None, None),
        P("tp"),
        P("tp", "fs"),
        P(),
        P("fs", "tp"),
        P("fs", "tp"),
        P(None, "tp"),
        P("tp", "fs"),
    )
    out_specs = P(("fs", "tp"), None)
    body = functools.partial(shards, mesh.shape["tp"])
    return jax.shard_map(body, mesh=mesh, in_specs=in_specs, out_specs=out_specs, check_vma=False)
```
